512 devices in a mesh: ep: 128 (over z, y, core), tp: 4 (over x).
Axes of the slice: x: 4, y: 8, z: 8, core: 2. Of those that a mesh axis runs over, the one named last changes fastest.
Arguments:
- tokens: bfloat16 [16384, 2048], P('ep'), may hold values from -24 to 24
- cotangent: bfloat16 [16384, 2048], P('ep'), may hold values from -6 to 6
- routing: int32 [16384, 2], P('ep'), may hold values from 0 to 127, all different within a row; in each aligned block of 128 rows (0 to 127, 128 to 255, ...) at most 4 rows name the same one
- router_weight: bfloat16 [2048, 128], replicated, may hold values from -0.125 to 0.125
- gate_weight: bfloat16 [128, 2048, 512], P('ep', None, 'tp'), may hold values from -0.125 to 0.125
- up_weight: bfloat16 [128, 2048, 512], P('ep', None, 'tp'), may hold values from -0.125 to 0.125
- down_weight: bfloat16 [128, 512, 2048], P('ep', 'tp'), may hold values from -0.25 to 0.25
Outputs:
- grad_tokens: bfloat16 [16384, 2048], P('ep', 'tp')
- grad_gating: float32 [16384, 2], P('ep')
- grad_router: float32 [2048, 128], P('ep')
- grad_gate_weight: bfloat16 [128, 2048, 512], P('ep', None, 'tp')
- grad_up_weight: bfloat16 [128, 2048, 512], P('ep', None, 'tp')
- grad_down_weight: bfloat16 [128, 512, 2048], P('ep', 'tp')
- in_norms: float32 [128, 2, 2048], P('ep')
- down_norms: float32 [128, 512], P('ep', 'tp')
- router_norms: float32 [2048], P('ep')
The draws below stay inside these ranges and needn't reach their ends.
Inputs may be any that keep to these rules, and one draw needn't show every extreme that they name: `routing`: each row names 2 different experts. Among the rows of one index of ep no expert is named by more than 4 rows, a bound that some block reaches in some of them.
All inputs are finite; a program needn't handle non-finite values.
Results may differ from the reference program's by a relative error of at most 0.014.
Values may be sent and summed in bfloat16 or wider, within the bound.
A program may use at most 64 MiB of HBM per device.

```python
import math
import jax
import jax.numpy as jnp
import numpy as np
from jax import lax

D = 2048
F = 512
TOP = 2
TOK_DEV = 128
EXPERTS = 128
TOKENS = 16384
CAP = 4
N_EP = 128
N_TP = 4


def raised(values, rng, source, target, shards_of, factor):
    owner, partner = [(jnp.arange(values.shape[dim]) // (values.shape[dim] // shards_of)).reshape([-1 if axis == dim else 1 for axis in range(values.ndim)]) for dim in (source, target)]
    chosen = jax.random.permutation(rng, shards_of)[partner]
    strong = (owner == chosen) | (owner == (partner + shards_of // 2) % shards_of)
    return jnp.where(strong, factor * values, values)


def level_of(stream_key, shape, pieces, smallest, largest):
    def one(dim, shards_of):
        heights = jax.random.uniform(jax.random.fold_in(jax.random.fold_in(stream_key, 6), dim), (shards_of,), jnp.float32, smallest / len(pieces), largest / len(pieces))
        return jnp.repeat(jnp.exp(heights), shape[dim] // shards_of).reshape((-1,) + (1,) * (len(shape) - dim - 1))

    level = one(*pieces[0])
    for cut in pieces[1:]:
        level = level * one(*cut)
    return level


def routed_block(stream_key, own, number, rows, number_of, top, bound, slope):
    ranking = jax.random.permutation(stream_key, number_of)
    packed, usual = shares(number_of, rows * top, bound, slope, True), shares(number_of, rows * top, bound, slope, False)
    places = jnp.arange(number_of)

    def named(sizes, turn):
        used = int((sizes > 0).sum())
        fixed = max(1, used // 4)
        shifted = fixed + (places - fixed + turn * (used - fixed)) % max(1, number_of - fixed)
        return jnp.zeros((number_of,), jnp.int32).at[ranking[jnp.where(places < fixed, places, shifted)]].set(jnp.asarray(sizes, jnp.int32))

    sizes = jnp.where(number % 4 == 0, named(packed, number // 4), named(usual, number - number // 4 - 1))
    mixed = jax.random.permutation(jax.random.fold_in(own, 3), number_of)
    donor, receiver = mixed[0:number_of // 2 * 2:2], mixed[1:number_of // 2 * 2:2]
    room = jnp.minimum(sizes[donor] - 1, bound - sizes[receiver]) // 2
    room = jnp.where((donor == ranking[0]) | (receiver == ranking[0]) | (sizes[receiver] == 0), 0, jnp.maximum(room, 0))
    shifted = jax.random.randint(jax.random.fold_in(own, 4), (number_of // 2,), 0, 1 << 20) % (room + 1)
    sizes = sizes.at[donor].add(-shifted).at[receiver].add(shifted)
    members = jnp.searchsorted(jnp.cumsum(sizes), jnp.arange(rows * top), side="right").astype(jnp.int32)
    listing = members.reshape(top, rows).T
    listing = listing[jax.random.permutation(jax.random.fold_in(own, 1), rows)]
    turn = jax.random.randint(jax.random.fold_in(own, 2), (rows, 1), 0, top)
    return jnp.take_along_axis(listing, (jnp.arange(top)[None, :] + turn) % top, axis=1)


def shares(count, total, limit, slope, full):
    portions = [(1 << 20) // math.isqrt(rank ** slope) + 1 for rank in range(1, count + 1)]
    largest = limit if full else min(limit, max(-(-total // count), total * portions[0] // sum(portions)))
    least = 1 if total - largest >= count - 1 else 0
    counts, surplus = [largest] + [least] * (count - 1), total - largest - least * (count - 1)
    while surplus > 0:
        movable = [i for i in range(1, count) if counts[i] < largest] or [i for i in range(1, count) if counts[i] < limit]
        whole, budget = sum([portions[i] for i in movable]), surplus
        for i in movable:
            addition = min(limit - counts[i], max(1, budget * portions[i] // whole), surplus)
            counts[i] = counts[i] + addition
            surplus = surplus - addition
    return np.array(counts)


def centred(stream_key, extent, scale, bound, cuts=(), held_as=jnp.bfloat16):
    values = scale * jax.random.normal(stream_key, extent, jnp.float32)
    if cuts:
        values = values * level_of(stream_key, extent, cuts, -0.22, 0.18)
    return jnp.clip(values, -bound, bound).astype(held_as)


def gaussian_with(own_key, extent, scale, reach, split, heavy, held_as=jnp.bfloat16):
    drawn = scale * jax.random.normal(own_key, extent, jnp.float32)
    if split:
        drawn = drawn * level_of(own_key, extent, split, -0.22, 0.18)
    return jnp.clip(raised(drawn, jax.random.fold_in(own_key, 3), *heavy), -reach, reach).astype(held_as)


def setup_inputs(seed: int = 0) -> dict:
    arg_keys = jax.random.split(jax.random.key(seed), 8)
    tokens = gaussian_with(arg_keys[0], (TOKENS, D), 1.0, 24.0, ((0, 128),), (0, 1, 128, 5.5))
    cotangent = centred(arg_keys[1], (TOKENS, D), 1.0, 6.0, ((0, 128),))
    routing_keys = jax.random.split(jax.random.fold_in(arg_keys[2], 1), TOKENS // TOK_DEV)
    routing_turns = jax.random.permutation(jax.random.fold_in(arg_keys[2], 3), TOKENS // TOK_DEV)
    routing = jax.vmap(lambda own, number: routed_block(jax.random.fold_in(arg_keys[2], 2), own, number, TOK_DEV, EXPERTS, TOP, CAP, 2))(routing_keys, routing_turns).reshape((TOKENS, TOP))
    router_weight = centred(arg_keys[3], (D, EXPERTS), D ** -0.5, 0.125)
    gate_weight = centred(arg_keys[4], (EXPERTS, D, F), D ** -0.5, 0.125, ((0, 128), (2, 4)))
    up_weight = centred(arg_keys[5], (EXPERTS, D, F), D ** -0.5, 0.125, ((0, 128), (2, 4)))
    down_weight = centred(arg_keys[6], (EXPERTS, F, D), F ** -0.5, 0.25, ((0, 128), (1, 4)))
    return {"tokens": tokens, "cotangent": cotangent, "routing": routing, "router_weight": router_weight, "gate_weight": gate_weight, "up_weight": up_weight, "down_weight": down_weight}


def silu_parts(pre_gate):
    sigmoid_gate = jax.nn.sigmoid(pre_gate)
    return pre_gate * sigmoid_gate, sigmoid_gate * (1.0 + pre_gate * (1.0 - sigmoid_gate))


def block_layout(block_routing):
    flat_expert = block_routing.reshape(-1)
    one_hot = (flat_expert[:, None] == jnp.arange(EXPERTS, dtype=jnp.int32)[None, :]).astype(jnp.int32)
    earlier = jnp.cumsum(one_hot, axis=0) - one_hot
    within = jnp.sum(earlier * one_hot, axis=1)
    position = (flat_expert * CAP + within).astype(jnp.int32)
    vacant = jnp.full((EXPERTS * CAP,), -1, jnp.int32)
    return vacant.at[position].set(jnp.arange(TOK_DEV * TOP, dtype=jnp.int32))


def reference(tokens, cotangent, routing, router_weight, gate_weight, up_weight, down_weight):
    local_layout = jax.vmap(block_layout)(routing.reshape(N_EP, TOK_DEV, TOP))
    offsets = (jnp.arange(N_EP, dtype=jnp.int32) * (TOK_DEV * TOP))[:, None]
    global_layout = jnp.where(local_layout >= 0, local_layout + offsets, TOKENS * TOP).astype(jnp.int32)
    expert_layout = global_layout.reshape(N_EP, EXPERTS, CAP).transpose(1, 0, 2).reshape(EXPERTS, N_EP * CAP)

    logits = jnp.dot(tokens, router_weight, preferred_element_type=jnp.float32)
    scores = jax.nn.sigmoid(jnp.take_along_axis(logits, routing, axis=1))
    score_sum = jnp.sum(scores, axis=1, keepdims=True)
    gating = scores / score_sum
    flat_gating = jnp.concatenate([gating.reshape(-1), jnp.zeros((1,), jnp.float32)])
    padded_tokens = jnp.concatenate([tokens, jnp.zeros((1, D), jnp.bfloat16)], axis=0)
    padded_cotangent = jnp.concatenate([cotangent, jnp.zeros((1, D), jnp.bfloat16)], axis=0)
    hidden_block = F // N_TP
    arrived = N_EP * CAP

    def one_expert(carried, inputs):
        token_terms, gating_grads = carried
        slot_layout, weight_gate, weight_up, weight_down = inputs
        source_rows = slot_layout // TOP
        rows_in = padded_tokens[source_rows]
        cot_rows = padded_cotangent[source_rows]
        slot_gating = flat_gating[slot_layout][:, None]
        pre_gate = jnp.dot(rows_in, weight_gate, preferred_element_type=jnp.float32)
        pre_up = jnp.dot(rows_in, weight_up, preferred_element_type=jnp.float32)
        activated, silu_slope = silu_parts(pre_gate)
        hidden = (activated * pre_up).astype(jnp.bfloat16)
        back_raw = lax.dot_general(cot_rows, weight_down, (((1,), (1,)), ((), ())),
                                   preferred_element_type=jnp.float32)
        hidden_wide = hidden.astype(jnp.float32)
        gate_grad = jnp.sum(hidden_wide * back_raw, axis=1)
        scaled_back = slot_gating * back_raw
        grad_pre_gate = (scaled_back * pre_up * silu_slope).astype(jnp.bfloat16)
        grad_pre_up = (scaled_back * activated).astype(jnp.bfloat16)
        scaled_hidden = (slot_gating * hidden_wide).astype(jnp.bfloat16)
        gate_sum = jnp.dot(rows_in.T, grad_pre_gate, preferred_element_type=jnp.float32)
        up_sum = jnp.dot(rows_in.T, grad_pre_up, preferred_element_type=jnp.float32)
        down_sum = jnp.dot(scaled_hidden.T, cot_rows, preferred_element_type=jnp.float32)
        norms_in = jnp.stack([jnp.sum(gate_sum * gate_sum, axis=1), jnp.sum(up_sum * up_sum, axis=1)])
        norms_down = jnp.sum(down_sum * down_sum, axis=1)
        pieces_gate = grad_pre_gate.reshape(arrived, N_TP, hidden_block).astype(jnp.float32)
        pieces_up = grad_pre_up.reshape(arrived, N_TP, hidden_block).astype(jnp.float32)
        blocks_gate = weight_gate.reshape(D, N_TP, hidden_block).astype(jnp.float32)
        blocks_up = weight_up.reshape(D, N_TP, hidden_block).astype(jnp.float32)
        partial_value = (jnp.einsum("rpf,dpf->prd", pieces_gate, blocks_gate)
                   + jnp.einsum("rpf,dpf->prd", pieces_up, blocks_up))
        rounded = lax.optimization_barrier(partial_value.astype(jnp.bfloat16))
        token_term = jnp.sum(rounded.astype(jnp.float32), axis=0).astype(jnp.bfloat16)
        token_terms = token_terms.at[slot_layout].set(token_term)
        gating_grads = gating_grads.at[slot_layout].set(gate_grad)
        return (token_terms, gating_grads), (gate_sum.astype(jnp.bfloat16), up_sum.astype(jnp.bfloat16),
                                             down_sum.astype(jnp.bfloat16), norms_in, norms_down)

    start_terms = jnp.zeros((TOKENS * TOP + 1, D), jnp.bfloat16)
    start_grads = jnp.zeros((TOKENS * TOP + 1,), jnp.float32)
    (token_terms, gating_grads), stacked = lax.scan(
        one_expert, (start_terms, start_grads), (expert_layout, gate_weight, up_weight, down_weight))
    grad_gate_weight, grad_up_weight, grad_down_weight, in_norms, down_norms = stacked

    summed_terms = jnp.sum(token_terms[:TOKENS * TOP].reshape(TOKENS, TOP, D).astype(jnp.float32), axis=1)
    grad_gating = gating_grads[:TOKENS * TOP].reshape(TOKENS, TOP)
    weighted = jnp.sum(gating * grad_gating, axis=1, keepdims=True)
    grad_scores = (grad_gating - weighted) / score_sum
    grad_chosen = grad_scores * scores * (1.0 - scores)
    token_index = jnp.arange(TOKENS, dtype=jnp.int32)[:, None]
    grad_logits = jnp.zeros((TOKENS, EXPERTS), jnp.float32).at[token_index, routing].add(grad_chosen)
    grad_logits = grad_logits.astype(jnp.bfloat16)
    router_term = lax.dot_general(grad_logits, router_weight, (((1,), (1,)), ((), ())),
                                  preferred_element_type=jnp.float32)
    grad_tokens = (summed_terms + router_term).astype(jnp.bfloat16)
    grad_router = jnp.dot(tokens.T, grad_logits, preferred_element_type=jnp.float32)
    router_norms = jnp.sum(grad_router * grad_router, axis=1)
    return (grad_tokens, grad_gating, grad_router, grad_gate_weight, grad_up_weight, grad_down_weight,
            in_norms, down_norms, router_norms)
```

```python
import functools

import jax
import jax.numpy as jnp
from jax import lax
from jax.experimental import pallas as pl
from jax.experimental.pallas import tpu as pltpu
from jax.sharding import Mesh
from jax.sharding import PartitionSpec as P

AXES = ("ep_0", "ep_1", "ep_2", "tp")
EP = AXES[:3]
MESH = pl.DeviceIdType.MESH
CAP = 4
LANES = 128
F32 = jnp.float32
BF16 = jnp.bfloat16
HIGH = lax.Precision.HIGHEST


class Sizes:
    def __init__(self, shape, tokens, width, hidden):
        self.nz, self.ny, self.nc, self.nx = shape
        self.nj = self.ny * self.nc
        self.ne = self.nz * self.nj
        self.t = tokens
        self.d = width
        self.f = hidden
        self.sl = width // self.nx
        self.fb = self.sl // LANES
        self.ur = CAP * self.fb
        self.gs = LANES // self.ur
        self.ng = self.ne // self.gs
        self.rows = self.gs * CAP
        self.s = self.ne * CAP
        self.zs = self.nj * CAP
        near = []
        for step in range(1, self.nz // 2 + 1):
            near += [step] if 2 * step == self.nz else [step, self.nz - step]
        self.near = near


def iota(shape, dim):
    return lax.broadcasted_iota(jnp.int32, shape, dim)


def dot(a, b, dims=((1,), (0,)), precision=None):
    return lax.dot_general(a, b, (dims, ((), ())), precision=precision, preferred_element_type=F32)


def to_unit(n):
    u, l = iota((LANES, LANES), 0), iota((LANES, LANES), 1)
    dev, fb, i = u // n.ur, (u // CAP) % n.fb, u % CAP
    return jnp.where(l == fb * n.rows + dev * CAP + i, 1.0, 0.0).astype(BF16)


def to_linear(n):
    u, l = iota((LANES, LANES), 1), iota((LANES, LANES), 0)
    dev, fb, i = u // n.ur, (u // CAP) % n.fb, u % CAP
    return jnp.where(l == fb * n.rows + dev * CAP + i, 1.0, 0.0).astype(BF16)


def stacked(n, block):
    return jnp.concatenate([block[:, b * LANES : (b + 1) * LANES] for b in range(n.fb)], axis=0)


def place(n):
    z, y = lax.axis_index(AXES[0]), lax.axis_index(AXES[1])
    c, x = lax.axis_index(AXES[2]), lax.axis_index(AXES[3])
    return z, y * n.nc + c, x


def wrap(value, size):
    return lax.rem(value, size)


def at_z(z):
    return {AXES[0]: z}


def at_j(n, j):
    return {AXES[1]: j // n.nc, AXES[2]: lax.rem(j, n.nc)}


def at_x(x):
    return {AXES[3]: x}


def greet(n):
    z, j, x = place(n)
    barrier = pltpu.get_barrier_semaphore()

    def tell(device):
        pl.semaphore_signal(barrier, inc=1, device_id=device, device_id_type=MESH)

    for dz in range(1, n.nz):
        tell(at_z(wrap(z + dz, n.nz)))

    @pl.loop(1, n.nj)
    def _(dj):
        tell(at_j(n, wrap(j + dj, n.nj)))

    for dx in range(1, n.nx):
        tell(at_x(wrap(x + dx, n.nx)))
    pl.semaphore_wait(barrier, n.nz + n.nj + n.nx - 3)


def remote(src, dst, send_sem, recv_sem, device):
    return pltpu.make_async_remote_copy(
        src_ref=src,
        dst_ref=dst,
        send_sem=send_sem,
        recv_sem=recv_sem,
        device_id=device,
        device_id_type=MESH,
    )


def wait_bytes(ref, sem):
    pltpu.make_async_copy(ref, ref, sem).wait()


def prepare(n, x, tok_ref, cot_ref, rout_ref, rw_ref, x_ref, g_ref, meta_ref):
    logits = dot(tok_ref[...], rw_ref[...])
    eio = iota((n.t, n.ne), 1)
    r0, r1 = rout_ref[:, 0:1], rout_ref[:, 1:2]
    oh0, oh1 = eio == r0, eio == r1
    s0 = jax.nn.sigmoid(jnp.sum(jnp.where(oh0, logits, 0.0), axis=1, keepdims=True))
    s1 = jax.nn.sigmoid(jnp.sum(jnp.where(oh1, logits, 0.0), axis=1, keepdims=True))
    total = s0 + s1
    g0, g1 = s0 / total, s1 / total
    f0, f1 = jnp.where(oh0, 1.0, 0.0), jnp.where(oh1, 1.0, 0.0)
    a, b = iota((n.t, n.t), 0), iota((n.t, n.t), 1)
    before = jnp.where(b < a, 1.0, 0.0).astype(BF16)
    c0 = dot(before, f0.astype(BF16))
    c1 = dot(before, f1.astype(BF16)) + jnp.sum(f0, axis=0, keepdims=True)
    w0 = jnp.sum(f0 * c0, axis=1, keepdims=True)
    w1 = jnp.sum(f1 * c1, axis=1, keepdims=True)
    r0f, r1f = r0.astype(F32), r1.astype(F32)
    columns = (r0f, r1f, w0, w1, g0, g1, s0, s1, total)
    lane = iota((n.t, LANES), 1)
    meta = jnp.zeros((n.t, LANES), F32)
    for k, column in enumerate(columns):
        meta = jnp.where(lane == k, column, meta)
    meta_ref[...] = meta
    lanef = lane.astype(F32)
    g_all = dot(f0, jnp.where(lanef == w0, g0, 0.0), ((0,), (0,)), HIGH) + dot(
        f1, jnp.where(lanef == w1, g1, 0.0), ((0,), (0,)), HIGH
    )
    for e in range(n.ne):
        g_ref[e] = g_all[e : e + 1, :]
    eye = a == b
    row0 = jnp.sum(jnp.where(eye, r0f * CAP + w0, 0.0), axis=0, keepdims=True)
    row1 = jnp.sum(jnp.where(eye, r1f * CAP + w1, 0.0), axis=0, keepdims=True)
    sio = iota((n.s, n.t), 0).astype(F32)
    pick = jnp.where((sio == row0) | (sio == row1), 1.0, 0.0).astype(BF16)
    unit = to_unit(n)
    mine = pl.ds(pl.multiple_of(x * n.sl, LANES), n.sl)
    for k, ref in enumerate((tok_ref, cot_ref)):
        lin = dot(pick, ref[:, mine]).astype(BF16)
        for g in range(n.ng):
            block = stacked(n, lin[g * n.rows : (g + 1) * n.rows, :])
            moved = dot(unit, block).astype(BF16)
            x_ref[g * n.gs : (g + 1) * n.gs, :, k * LANES : (k + 1) * LANES] = moved.reshape(
                n.gs, n.ur, LANES
            )


def dispatch_kernel(
    n, tok_ref, cot_ref, rout_ref, rw_ref,
    rt_ref, gt_ref, meta_ref,
    x_ref, g_ref, r_ref, gr_ref,
    zs, zr, gzs, gzr, ys, yr, gys, gyr, ls, gls, xs, xr, fs, fr,
):
    z, j, x = place(n)
    greet(n)
    prepare(n, x, tok_ref, cot_ref, rout_ref, rw_ref, x_ref, g_ref, meta_ref)
    right, left = wrap(x + 1, n.nx), wrap(x + n.nx - 1, n.nx)
    half = n.nj // 2

    def z_copies(dz):
        to = wrap(z + dz, n.nz)
        block = pl.ds(to * n.nj, n.nj)
        return (
            remote(x_ref.at[block], r_ref.at[dz], zs.at[dz], zr.at[dz], at_z(to)),
            remote(g_ref.at[block], gr_ref.at[dz], gzs.at[dz], gzr.at[dz], at_z(to)),
        )

    for dz in n.near:
        for copy in z_copies(dz):
            copy.start()

    def source(dz):
        return wrap(z + n.nz - dz, n.nz)

    def unit_of(dz, unit):
        if dz == 0:
            return x_ref.at[z * n.nj + unit], g_ref.at[z * n.nj + unit]
        return r_ref.at[dz, unit], gr_ref.at[dz, unit]

    def local_copies(dz):
        own, gown = unit_of(dz, j)
        to = source(dz) * n.nj + j
        return (
            pltpu.make_async_copy(own, rt_ref.at[x, to], ls.at[dz]),
            pltpu.make_async_copy(gown, gt_ref.at[to], gls.at[dz]),
        )

    def y_stage(dz):
        if dz:
            for copy in z_copies(dz):
                copy.wait_recv()
        for copy in local_copies(dz):
            copy.start()
        to = source(dz) * n.nj + j

        @pl.loop(1, n.nj)
        def _(dj):
            other = wrap(j + dj, n.nj)
            unit, gunit = unit_of(dz, other)
            remote(unit, rt_ref.at[x, to], ys.at[dz], yr.at[dz], at_j(n, other)).start()
            remote(gunit, gt_ref.at[to], gys.at[dz], gyr.at[dz], at_j(n, other)).start()

    def chunk(dz, owner, first, count):
        return rt_ref.at[owner, pl.ds(source(dz) * n.nj + first, count)]

    def x_copies(dz):
        own = chunk(dz, x, 0, n.nj)
        return (
            remote(own, own, xs.at[0, dz], xr.at[0, dz], at_x(right)),
            remote(own, own, xs.at[1, dz], xr.at[1, dz], at_x(left)),
        )

    def x_stage(dz):
        for copy in local_copies(dz):
            copy.wait()
        wait_bytes(chunk(dz, x, 0, n.nj - 1), yr.at[dz])
        wait_bytes(gt_ref.at[pl.ds(0, n.nj - 1)], gyr.at[dz])
        for copy in x_copies(dz):
            copy.start()

    def forward_copies(dz):
        one, two = chunk(dz, left, 0, half), chunk(dz, right, half, n.nj - half)
        return (
            remote(one, one, fs.at[0, dz], fr.at[0, dz], at_x(right)),
            remote(two, two, fs.at[1, dz], fr.at[1, dz], at_x(left)),
        )

    def f_stage(dz):
        for copy, forward in zip(x_copies(dz), forward_copies(dz)):
            copy.wait_recv()
            forward.start()

    def done(dz):
        for copy in forward_copies(dz):
            copy.wait_recv()

    order = [0] + n.near
    stages = (y_stage, x_stage, f_stage, done)
    for step in range(n.nz + len(stages) - 1):
        for k, stage in enumerate(stages):
            if 0 <= step - k < n.nz:
                stage(order[step - k])
    for dz in order:
        if dz:
            for copy in z_copies(dz):
                copy.wait_send()
        wait_bytes(chunk(dz, x, 0, n.nj - 1), ys.at[dz])
        wait_bytes(gt_ref.at[pl.ds(0, n.nj - 1)], gys.at[dz])
        for copy in (*x_copies(dz), *forward_copies(dz)):
            copy.wait_send()


def dma(*shape):
    return pltpu.SemaphoreType.DMA(shape)


def vmem(*_):
    return pl.BlockSpec(memory_space=pltpu.VMEM)


def dispatch(n, tokens, cotangent, routing, router_weight):
    return pl.pallas_call(
        functools.partial(dispatch_kernel, n),
        name="dispatch",
        out_shape=(
            jax.ShapeDtypeStruct((n.nx, n.ne, n.ur, 2 * LANES), BF16),
            jax.ShapeDtypeStruct((n.ne, 1, LANES), F32),
            jax.ShapeDtypeStruct((n.t, LANES), F32),
        ),
        in_specs=[vmem()] * 4,
        out_specs=(vmem(), vmem(), vmem()),
        scratch_shapes=[
            pltpu.VMEM((n.ne, n.ur, 2 * LANES), BF16),
            pltpu.VMEM((n.ne, 1, LANES), F32),
            pltpu.VMEM((n.nz, n.nj, n.ur, 2 * LANES), BF16),
            pltpu.VMEM((n.nz, n.nj, 1, LANES), F32),
            *([dma(n.nz)] * 10),
            *([dma(2, n.nz)] * 4),
        ],
        compiler_params=pltpu.CompilerParams(collective_id=0, has_side_effects=True),
    )(tokens, cotangent, routing, router_weight)


def expert_kernel(
    n, rt_ref, gt_ref, wg_ref, wu_ref, wd_ref,
    gg_ref, gu_ref, gd_ref, dn_ref, back_ref, gp_ref, nrm_ref,
    rows_ref, cots_ref, w_ref,
):
    hid = n.f
    lin = to_linear(n)

    @pl.loop(0, n.ng)
    def _(g):
        at = pl.ds(pl.multiple_of(g * n.rows, n.rows), n.rows)
        for k in range(n.nx):
            block = rt_ref[k, pl.ds(g * n.gs, n.gs)].reshape(LANES, 2 * LANES)
            moved = dot(lin, block).astype(BF16)
            for b in range(n.fb):
                part = moved[b * n.rows : (b + 1) * n.rows]
                lanes = pl.ds(k * n.sl + b * LANES, LANES)
                rows_ref[at, lanes] = part[:, :LANES]
                cots_ref[at, lanes] = part[:, LANES:]

    w_ref[:, :hid] = wg_ref[...]
    w_ref[:, hid:] = wu_ref[...]
    owner = iota((n.s, n.ne), 0) // CAP == iota((n.s, n.ne), 1)
    spread = dot(jnp.where(owner, 1.0, 0.0), gt_ref[:, 0, :], precision=HIGH)
    slot = iota((n.s, LANES), 0) % CAP == iota((n.s, LANES), 1)
    gating = jnp.sum(jnp.where(slot, spread, 0.0), axis=1, keepdims=True)

    rows, cots = rows_ref[...], cots_ref[...]
    pre = dot(rows, w_ref[...])
    pre_gate, pre_up = pre[:, :hid], pre[:, hid:]
    sig = jax.nn.sigmoid(pre_gate)
    activated = pre_gate * sig
    slope = sig * (1.0 + pre_gate * (1.0 - sig))
    hidden = (activated * pre_up).astype(BF16)
    back = dot(cots, wd_ref[...], ((1,), (1,)))
    wide = hidden.astype(F32)
    gp_ref[...] = dot(jnp.ones((8, hid), F32), wide * back, ((1,), (1,)), HIGH)
    scaled = gating * back
    grads = jnp.concatenate(
        [(scaled * pre_up * slope).astype(BF16), (scaled * activated).astype(BF16)], axis=1
    )
    scaled_hidden = (gating * wide).astype(BF16)
    back_ref[...] = dot(grads, w_ref[...], ((1,), (1,))).astype(BF16)
    both = dot(grads, rows, ((0,), (0,)))
    for k, ref in enumerate((gg_ref, gu_ref)):
        part = both[k * hid : (k + 1) * hid, :]
        nrm_ref[k : k + 1, :] = jnp.sum(part * part, axis=0, keepdims=True)
        ref[...] = part.T.astype(BF16)
    down = dot(scaled_hidden, cots, ((0,), (0,)))
    gd_ref[...] = down.astype(BF16)
    squares = jnp.sum(down * down, axis=1, keepdims=True)
    eye = iota((hid, hid), 0) == iota((hid, hid), 1)
    dn_ref[...] = jnp.sum(jnp.where(eye, squares, 0.0), axis=0, keepdims=True)


def experts(n, rt, gt, wg, wu, wd):
    def like(shape, dtype):
        return jax.ShapeDtypeStruct(shape, dtype)

    return pl.pallas_call(
        functools.partial(expert_kernel, n),
        name="experts",
        out_shape=(
            like((n.d, n.f), BF16),
            like((n.d, n.f), BF16),
            like((n.f, n.d), BF16),
            like((1, n.f), F32),
            like((n.s, n.d), BF16),
            like((8, n.s), F32),
            like((2, n.d), F32),
        ),
        in_specs=[vmem()] * 5,
        out_specs=tuple([vmem()] * 7),
        scratch_shapes=[
            pltpu.VMEM((n.s, n.d), BF16),
            pltpu.VMEM((n.s, n.d), BF16),
            pltpu.VMEM((n.d, 2 * n.f), BF16),
        ],
        compiler_params=pltpu.CompilerParams(vmem_limit_bytes=60 * 1024 * 1024),
    )(rt, gt, wg, wu, wd)


def return_kernel(
    n, back_ref, gp_ref, nrm_ref, meta_ref, tok_ref, rw_ref,
    gt_out, gg_out, gr_out, in_out, rn_out,
    gall_ref, nall_ref, rv_ref, y_ref, rz_ref, v_ref,
    h_ref, hz_ref, hv_ref, q_ref, qz_ref, qy_ref, qv_ref, u_ref,
    xgs, xgr, xns, xnr, xvs, xvr, zvs, zvr, yvs, yvr, lvs,
    zgs, zgr, ygs, ygr, lgs, zqs, zqr, yqs, yqr, xqs, xqr,
):
    z, j, x = place(n)
    others = range(1, n.nx)
    far = n.near[::-1] + [0]
    greet(n)

    def sink(dz):
        return wrap(z + dz, n.nz)

    def source(dz):
        return wrap(z + n.nz - dz, n.nz)

    gall_ref[x] = gp_ref[0:1, :]
    nall_ref[x] = nrm_ref[...]

    def xg_copy(dx):
        to = wrap(x + dx, n.nx)
        return remote(gall_ref.at[x], gall_ref.at[x], xgs.at[dx], xgr.at[dx], at_x(to))

    def xn_copy(dx):
        to = wrap(x + dx, n.nx)
        return remote(nall_ref.at[x], nall_ref.at[x], xns.at[dx], xnr.at[dx], at_x(to))

    def rows_of(dz):
        return pl.ds(pl.multiple_of(sink(dz) * n.zs, n.zs), n.zs)

    def xv_copy(dz, dx):
        to = wrap(x + dx, n.nx)
        lanes = pl.ds(pl.multiple_of(to * n.sl, LANES), n.sl)
        return remote(
            back_ref.at[rows_of(dz), lanes], rv_ref.at[dx, dz],
            xvs.at[dx, dz], xvr.at[dx, dz], at_x(to),
        )

    for dx in others:
        xg_copy(dx).start()
    for dz in far:
        for dx in others:
            xv_copy(dz, dx).start()
    for dx in others:
        xn_copy(dx).start()

    def gate_home():
        for dx in others:
            xg_copy(dx).wait_recv()
        total = gall_ref[0]
        for k in others:
            total = total + gall_ref[k]
        keep = iota((n.ne, n.s), 1) // CAP == iota((n.ne, n.s), 0)
        lanes = iota((n.s, LANES), 0) % CAP == iota((n.s, LANES), 1)
        units = dot(
            jnp.where(keep, total, 0.0), jnp.where(lanes, 1.0, 0.0), precision=HIGH
        )
        for e in range(n.ne):
            h_ref[e] = units[e : e + 1, :]
        for dz in n.near:
            zg_copy(dz).start()

    def zg_copy(dz):
        block = pl.ds(sink(dz) * n.nj, n.nj)
        return remote(h_ref.at[block], hz_ref.at[dz], zgs.at[dz], zgr.at[dz], at_z(sink(dz)))

    def gate_unit(dz, unit):
        return h_ref.at[z * n.nj + unit] if dz == 0 else hz_ref.at[dz, unit]

    def gate_local(dz):
        return pltpu.make_async_copy(
            gate_unit(dz, j), hv_ref.at[source(dz) * n.nj + j], lgs.at[dz]
        )

    def gate_y():
        for dz in [0] + n.near:
            if dz:
                zg_copy(dz).wait_recv()
            gate_local(dz).start()
            to = source(dz) * n.nj + j

            @pl.loop(1, n.nj)
            def _(dj):
                other = wrap(j + dj, n.nj)
                remote(
                    gate_unit(dz, other), hv_ref.at[to], ygs.at[dz], ygr.at[dz], at_j(n, other)
                ).start()

    meta = meta_ref[...]

    def column(k):
        return meta[:, k : k + 1]

    eio = iota((n.t, n.ne), 1).astype(F32)
    oh0, oh1 = eio == column(0), eio == column(1)

    def gate_final():
        for dz in range(n.nz):
            gate_local(dz).wait()
            wait_bytes(hv_ref.at[pl.ds(0, n.nj - 1)], ygr.at[dz])
        home = hv_ref[:, 0, :]
        lanef = iota((n.t, LANES), 1).astype(F32)
        parts = []
        for oh, within in ((oh0, column(2)), (oh1, column(3))):
            got = dot(jnp.where(oh, 1.0, 0.0), home, precision=HIGH)
            parts.append(jnp.sum(jnp.where(lanef == within, got, 0.0), axis=1, keepdims=True))
        gg0, gg1 = parts
        k2 = iota((n.t, 2), 1)
        gg_out[...] = jnp.where(k2 == 0, gg0, gg1)
        weighted = column(4) * gg0 + column(5) * gg1
        s0, s1, total = column(6), column(7), column(8)
        c0 = (gg0 - weighted) / total * s0 * (1.0 - s0)
        c1 = (gg1 - weighted) / total * s1 * (1.0 - s1)
        return (jnp.where(oh0, c0, 0.0) + jnp.where(oh1, c1, 0.0)).astype(BF16)

    part_rows = n.d // n.ne
    quarter = part_rows // n.nx

    def zq_copy(dz):
        return remote(q_ref.at[sink(dz)], qz_ref.at[dz], zqs.at[dz], zqr.at[dz], at_z(sink(dz)))

    def router_z(grad_logits):
        full = dot(tok_ref[...], grad_logits, ((0,), (0,)))
        full = full.reshape(n.ne, part_rows, n.ne)
        mine = full[:, :quarter, :]
        for k in others:
            mine = jnp.where(x == k, full[:, k * quarter : (k + 1) * quarter, :], mine)
        q_ref[...] = mine.reshape(n.nz, n.nj, quarter, n.ne)
        for dz in n.near:
            zq_copy(dz).start()

    def yq_copy(dj):
        to = wrap(j + dj, n.nj)
        return remote(u_ref.at[to], qy_ref.at[dj], yqs, yqr, at_j(n, to))

    def router_y():
        total = q_ref[z]
        for dz in n.near:
            zq_copy(dz).wait_recv()
            total = total + qz_ref[dz]
        u_ref[...] = total

        @pl.loop(1, n.nj)
        def _(dj):
            yq_copy(dj).start()

    def xq_copy(dx):
        to = wrap(x + dx, n.nx)
        return remote(qv_ref.at[x], qv_ref.at[x], xqs.at[dx], xqr.at[dx], at_x(to))

    def router_x():
        wait_bytes(qy_ref.at[pl.ds(1, n.nj - 1)], yqr)
        total = u_ref[j]
        for dj in range(1, n.nj):
            total = total + qy_ref[dj]
        qv_ref[x] = total
        for dx in others:
            xq_copy(dx).start()

    def router_final():
        for dx in others:
            xq_copy(dx).wait_recv()
        for k in range(n.nx):
            block = qv_ref[k]
            gr_out[k * quarter : (k + 1) * quarter, :] = block
            square = jnp.sum(block * block, axis=1, keepdims=True)
            rn_out[k * quarter : (k + 1) * quarter, :] = jnp.broadcast_to(square, block.shape)

    unit = to_unit(n)

    def zv_copy(dz):
        return remote(y_ref.at[dz], rz_ref.at[dz], zvs.at[dz], zvr.at[dz], at_z(sink(dz)))

    def values_z(dz):
        own = pl.ds(pl.multiple_of(x * n.sl, LANES), n.sl)
        total = back_ref[rows_of(dz), own].astype(F32)
        for dx in others:
            xv_copy(dz, dx).wait_recv()
            total = total + rv_ref[dx, dz].astype(F32)
        total = total.astype(BF16)
        for g in range(n.zs // n.rows):
            moved = dot(unit, stacked(n, total[g * n.rows : (g + 1) * n.rows])).astype(BF16)
            y_ref[dz, g * n.gs : (g + 1) * n.gs] = moved.reshape(n.gs, n.ur, LANES)
        if dz:
            zv_copy(dz).start()

    def value_unit(dz, which):
        return y_ref.at[0, which] if dz == 0 else rz_ref.at[dz, which]

    def value_local(dz):
        return pltpu.make_async_copy(
            value_unit(dz, j), v_ref.at[source(dz) * n.nj + j], lvs.at[dz]
        )

    def values_y(dz):
        if dz:
            zv_copy(dz).wait_recv()
        value_local(dz).start()
        to = source(dz) * n.nj + j

        @pl.loop(1, n.nj)
        def _(dj):
            other = wrap(j + dj, n.nj)
            remote(
                value_unit(dz, other), v_ref.at[to], yvs.at[dz], yvr.at[dz], at_j(n, other)
            ).start()

    gate_home()
    grad_logits = None
    for step in range(n.nz + 1):
        if step < n.nz:
            values_z(far[step])
        if step:
            values_y(far[step - 1])
        if step == 0:
            gate_y()
        if step == 2 * n.nz // 8:
            grad_logits = gate_final()
            router_z(grad_logits)
        if step == 4 * n.nz // 8:
            router_y()
        if step == 6 * n.nz // 8:
            router_x()
    for dx in others:
        xn_copy(dx).wait_recv()
    total = nall_ref[0]
    for k in others:
        total = total + nall_ref[k]
    in_out[...] = total
    router_term = dot(
        grad_logits, rw_ref[pl.ds(pl.multiple_of(x * n.sl, n.sl), n.sl), :], ((1,), (1,))
    )
    router_final()
    for dz in range(n.nz):
        value_local(dz).wait()
        wait_bytes(v_ref.at[pl.ds(0, n.nj - 1)], yvr.at[dz])
    lin = to_linear(n)
    slots = []
    for g in range(n.ng):
        moved = dot(lin, v_ref[g * n.gs : (g + 1) * n.gs].reshape(LANES, LANES)).astype(BF16)
        slots.append(
            jnp.concatenate(
                [moved[b * n.rows : (b + 1) * n.rows] for b in range(n.fb)], axis=1
            )
        )
    slots = jnp.concatenate(slots, axis=0)
    sio = iota((n.t, n.s), 1).astype(F32)
    slot0, slot1 = column(0) * CAP + column(2), column(1) * CAP + column(3)
    pick = jnp.where((sio == slot0) | (sio == slot1), 1.0, 0.0).astype(BF16)
    gt_out[...] = (dot(pick, slots) + router_term).astype(BF16)

    for dx in others:
        for copy in (xg_copy(dx), xn_copy(dx), xq_copy(dx)):
            copy.wait_send()
        for dz in range(n.nz):
            xv_copy(dz, dx).wait_send()
    for dz in range(n.nz):
        if dz:
            for copy in (zg_copy(dz), zq_copy(dz), zv_copy(dz)):
                copy.wait_send()
        wait_bytes(hv_ref.at[pl.ds(0, n.nj - 1)], ygs.at[dz])
        wait_bytes(v_ref.at[pl.ds(0, n.nj - 1)], yvs.at[dz])
    wait_bytes(qy_ref.at[pl.ds(1, n.nj - 1)], yqs)


def back_home(n, back, gp, nrm, meta, tokens, router_weight):
    part_rows = n.d // n.ne
    quarter = part_rows // n.nx

    def like(shape, dtype):
        return jax.ShapeDtypeStruct(shape, dtype)

    return pl.pallas_call(
        functools.partial(return_kernel, n),
        name="back_home",
        out_shape=(
            like((n.t, n.sl), BF16),
            like((n.t, 2), F32),
            like((part_rows, n.ne), F32),
            like((2, n.d), F32),
            like((part_rows, n.ne), F32),
        ),
        in_specs=[vmem()] * 6,
        out_specs=tuple([vmem()] * 5),
        scratch_shapes=[
            pltpu.VMEM((n.nx, 1, n.s), F32),
            pltpu.VMEM((n.nx, 2, n.d), F32),
            pltpu.VMEM((n.nx, n.nz, n.zs, n.sl), BF16),
            pltpu.VMEM((n.nz, n.nj, n.ur, LANES), BF16),
            pltpu.VMEM((n.nz, n.nj, n.ur, LANES), BF16),
            pltpu.VMEM((n.ne, n.ur, LANES), BF16),
            pltpu.VMEM((n.ne, 1, LANES), F32),
            pltpu.VMEM((n.nz, n.nj, 1, LANES), F32),
            pltpu.VMEM((n.ne, 1, LANES), F32),
            pltpu.VMEM((n.nz, n.nj, quarter, n.ne), F32),
            pltpu.VMEM((n.nz, n.nj, quarter, n.ne), F32),
            pltpu.VMEM((n.nj, quarter, n.ne), F32),
            pltpu.VMEM((n.nx, quarter, n.ne), F32),
            pltpu.VMEM((n.nj, quarter, n.ne), F32),
            *([dma(n.nx)] * 4),
            *([dma(n.nx, n.nz)] * 2),
            *([dma(n.nz)] * 5),
            *([dma(n.nz)] * 7),
            pltpu.SemaphoreType.DMA,
            pltpu.SemaphoreType.DMA,
            *([dma(n.nx)] * 2),
        ],
        compiler_params=pltpu.CompilerParams(collective_id=1, has_side_effects=True),
    )(back, gp, nrm, meta, tokens, router_weight)


def shards(shape, tokens, cotangent, routing, router_weight, gate_weight, up_weight, down_weight):
    n = Sizes(shape, tokens.shape[0], tokens.shape[1], gate_weight.shape[2])
    rt, gt, meta = dispatch(n, tokens, cotangent, routing, router_weight)
    grad_gate, grad_up, grad_down, down_norms, back, gp, nrm = experts(
        n, rt, gt, gate_weight[0], up_weight[0], down_weight[0]
    )
    grad_tokens, grad_gating, grad_router, in_norms, router_norms = back_home(
        n, back, gp, nrm, meta, tokens, router_weight
    )
    return (
        grad_tokens,
        grad_gating,
        grad_router,
        grad_gate[None],
        grad_up[None],
        grad_down[None],
        in_norms[None],
        down_norms,
        router_norms[:, 0],
    )


def solution(mesh, shape=(8, 8, 2)):
    shape = (*shape, mesh.shape["tp"])
    split = Mesh(mesh.devices.reshape(shape), AXES)
    in_specs = (
        P(EP, None),
        P(EP, None),
        P(EP, None),
        P(),
        P(EP, None, "tp"),
        P(EP, None, "tp"),
        P(EP, "tp", None),
    )
    out_specs = (
        P(EP, "tp"),
        P(EP, None),
        P(EP, None),
        P(EP, None, "tp"),
        P(EP, None, "tp"),
        P(EP, "tp", None),
        P(EP, None, None),
        P(EP, "tp"),
        P(EP),
    )
    return jax.shard_map(
        functools.partial(shards, shape),
        mesh=split,
        in_specs=in_specs,
        out_specs=out_specs,
        check_vma=False,
    )
```
